32 devices in a mesh: grp: 2 (over y), fs: 4 (over z), tp: 4 (over x, core).
Axes of the slice: x: 2, y: 2, z: 4, core: 2. Of those that a mesh axis runs over, the one named last changes fastest.
Arguments:
- tokens: bfloat16 [3072, 2048], P(('grp', 'fs'), 'tp'), parts along dimension 0, may hold values from -6 to 6
- norm_gain: float32 [2048], P('fs'), may hold values from 0.1 to 1.9
- gate_weight: float32 [32, 2048, 1024], P(None, 'fs', 'tp'), may hold values from -0.125 to 0.125
- up_weight: float32 [32, 2048, 1024], P(None, 'fs', 'tp'), may hold values from -0.125 to 0.125
- down_weight: float32 [32, 1024, 2048], P(None, 'fs', 'tp'), may hold values from -0.1875 to 0.1875
- routes: int32 [3072, 2], P(('grp', 'fs')), parts along dimension 0, may hold values from 0 to 31, as said below
- route_weights: float32 [3072, 2], P(('grp', 'fs')), parts along dimension 0, may hold values from 0.2 to 1
Outputs:
- gate_serve: bfloat16 [64, 2048, 1024], P(('grp', 'fs'), None, 'tp'), parts along dimension 0
- up_serve: bfloat16 [64, 2048, 1024], P(('grp', 'fs'), None, 'tp'), parts along dimension 0
- down_serve: bfloat16 [64, 1024, 2048], P(('grp', 'fs'), None, 'tp'), parts along dimension 0
- mixture: bfloat16 [3072, 2048], P(('grp', 'fs'), 'tp'), parts along dimension 0
The draws below stay inside these ranges and needn't reach their ends.
There are 2 independent parts, one for each index of `grp`. The reference program is written for one: setup_inputs(seed, part) draws one part's arguments, and reference() takes and returns one part's arrays. A program takes and returns all parts, laid end to end along the dimension named above; an argument that names none is the same for every part. Nothing has to cross between parts.
Inputs may be any that keep to these rules, and one draw needn't show every extreme that they name: `routes`: each row names two different experts of one group (expert e lies in group e // 8). In each aligned block of 384 rows no expert is named more than 36 times, and every expert of one group is named exactly 36 times.
All inputs are finite; a program needn't handle non-finite values.
Results may differ from the reference program's by a relative error of at most 0.0087.
Values may be sent and summed in bfloat16 or wider, within the bound.
A program may use at most 192 MiB of HBM per device.

```python
import jax
import jax.numpy as jnp
from jax import lax

D = 2048
DE = 1024
NGROUPS = 4
EPG = 8
TOK_DEV = 384
EXPERTS = 32
CAP = 36
TOKENS = 1536


def block_routes(block_key):
    subkeys = jax.random.split(block_key, 6)
    eighth = TOK_DEV // 8
    first_count = jax.random.randint(subkeys[0], (), eighth, 2 * eighth + 1, dtype=jnp.int32)
    second_count = jax.random.randint(subkeys[1], (), eighth, 2 * eighth + 1, dtype=jnp.int32)
    counts = jnp.stack([jnp.int32(3 * eighth), first_count, second_count, jnp.int32(5 * eighth) - first_count - second_count]).astype(jnp.int32)
    starts = (jnp.cumsum(counts) - counts).astype(jnp.int32)
    places = jnp.arange(TOK_DEV, dtype=jnp.int32)
    order_slot = jnp.sum((places[:, None] >= starts[None, 1:]).astype(jnp.int32), axis=1).astype(jnp.int32)
    rank_in_group = places - starts[order_slot]
    group_order = jax.random.permutation(subkeys[2], NGROUPS).astype(jnp.int32)
    group_id = group_order[order_slot]
    member_keys = jax.random.split(subkeys[3], NGROUPS)
    member_perm = jax.vmap(lambda member_key: jax.random.permutation(member_key, EPG))(member_keys).astype(jnp.int32)
    shifts = jax.random.randint(subkeys[4], (NGROUPS, TOK_DEV // EPG + 1), 0, EPG - 1, dtype=jnp.int32)
    lead_member = rank_in_group % EPG
    partner = (rank_in_group + 1 + shifts[order_slot, rank_in_group // EPG]) % EPG
    first_expert = group_id * EPG + member_perm[group_id, lead_member]
    second_expert = group_id * EPG + member_perm[group_id, partner]
    expert_pairs = jnp.stack([first_expert, second_expert], axis=1).astype(jnp.int32)
    shuffle = jax.random.permutation(subkeys[5], TOK_DEV).astype(jnp.int32)
    return jnp.zeros((TOK_DEV, 2), jnp.int32).at[shuffle].set(expert_pairs)


def draw_routes(key, part):
    block_keys = jax.random.split(jax.random.fold_in(key, 17), TOKENS // TOK_DEV)
    return jax.vmap(block_routes)(block_keys).reshape(TOKENS, 2).astype(jnp.int32)


def level_of(rng, shape, shards, smallest, high):
    factor_of = 1.0
    for dim, parts in shards:
        steps = jax.random.uniform(jax.random.fold_in(jax.random.fold_in(rng, 6), dim), (parts,), jnp.float32, smallest / len(shards), high / len(shards))
        factor_of = factor_of * jnp.repeat(jnp.exp(steps), shape[dim] // parts).reshape((-1,) + (1,) * (len(shape) - 1 - dim))
    return factor_of


def normal_values(rng, dims, scale, bound, shards=(), held_as=jnp.bfloat16):
    array = scale * jax.random.normal(rng, dims, jnp.float32)
    if shards:
        array = array * level_of(rng, dims, shards, -0.22, 0.18)
    return jnp.clip(array, -bound, bound).astype(held_as)


def setup_inputs(seed: int = 0, part: int = 0) -> dict:
    splits = jax.random.split(jax.random.key(seed), 8)
    part_keys = jax.random.split(jax.random.fold_in(splits[7], part), 8)
    return {
        "tokens": normal_values(part_keys[0], (TOKENS, D), 1.0, 6.0, ((0, 4), (1, 4))),
        "norm_gain": jnp.clip(1.0 + 0.18 * jax.random.normal(splits[1], (D,), jnp.float32), 0.1, 1.9),
        "gate_weight": normal_values(splits[2], (EXPERTS, D, DE), D ** -0.5, 0.125, ((1, 4), (2, 4)), jnp.float32),
        "up_weight": normal_values(splits[3], (EXPERTS, D, DE), D ** -0.5, 0.125, ((1, 4), (2, 4)), jnp.float32),
        "down_weight": normal_values(splits[4], (EXPERTS, DE, D), DE ** -0.5, 0.1875, ((1, 4), (2, 4)), jnp.float32),
        "routes": draw_routes(jax.random.fold_in(jax.random.fold_in(splits[7], part), 71), part),
        "route_weights": jnp.clip(0.2 + 0.8 * jax.random.uniform(part_keys[6], (TOKENS, 2), jnp.float32) ** level_of(part_keys[6], (TOKENS, 2), ((0, 4),), -0.2, 0.2), 0.2, 1.0),
    }


epsilon = 1e-06

def normalize(rows):
    values = rows.astype(jnp.float32)
    scale = lax.rsqrt(lax.optimization_barrier(jnp.mean(values * values, axis=-1, keepdims=True)) + epsilon)
    return (values * scale).astype(jnp.bfloat16)

def reference(tokens, norm_gain, gate_weight, up_weight, down_weight, routes, route_weights):
    gate_serve = (norm_gain[None, :, None] * gate_weight).astype(jnp.bfloat16)
    up_serve = (norm_gain[None, :, None] * up_weight).astype(jnp.bfloat16)
    down_serve = down_weight.astype(jnp.bfloat16)
    normed = normalize(tokens)
    blocks = TOKENS // TOK_DEV
    span = blocks * CAP
    flat_routes = routes.reshape(blocks, TOK_DEV * 2)
    expert_ids = jnp.arange(EXPERTS, dtype=jnp.int32)
    onehot = (flat_routes[:, :, None] == expert_ids[None, None, :]).astype(jnp.int32)
    position = lax.optimization_barrier(jnp.sum((jnp.cumsum(onehot, axis=1) - 1) * onehot, axis=2)).astype(jnp.int32)
    block_ids = jnp.arange(blocks, dtype=jnp.int32)[:, None]
    destination = (flat_routes * span + block_ids * CAP + position).astype(jnp.int32)
    token_ids = block_ids * TOK_DEV + (jnp.arange(TOK_DEV * 2, dtype=jnp.int32) // 2)[None, :]
    table = jnp.full((EXPERTS * span,), TOKENS, jnp.int32)
    table = table.at[destination.reshape(-1)].set(token_ids.reshape(-1).astype(jnp.int32))
    padded = jnp.concatenate([normed, jnp.zeros((1, D), jnp.bfloat16)], axis=0)

    def expert_rows(operands):
        index_rows, gate_matrix, up_matrix, down_matrix = operands
        rows = padded[index_rows]
        gate_part = jnp.dot(rows, gate_matrix, preferred_element_type=jnp.float32)
        up_part = jnp.dot(rows, up_matrix, preferred_element_type=jnp.float32)
        hidden = (jax.nn.silu(gate_part) * up_part).astype(jnp.bfloat16)
        return jnp.dot(hidden, down_matrix, preferred_element_type=jnp.float32).astype(jnp.bfloat16)
    outputs = lax.map(expert_rows, (table.reshape(EXPERTS, span), gate_serve, up_serve, down_serve))
    picked = outputs.reshape(EXPERTS * span, D)[destination.reshape(TOKENS, 2)]
    mixture = lax.optimization_barrier(jnp.sum(route_weights[:, :, None] * picked.astype(jnp.float32), axis=1)).astype(jnp.bfloat16)
    return (gate_serve, up_serve, down_serve, mixture)
```

```python
import jax
import jax.numpy as jnp
from jax import lax
from jax.sharding import PartitionSpec as P

CAP = 36
GROUP = 8


epsilon = 1e-06


def normalize(rows):
    values = rows.astype(jnp.float32)
    scale = lax.rsqrt(jnp.mean(values * values, axis=-1, keepdims=True) + epsilon)
    return (values * scale).astype(jnp.bfloat16)


def positions(ids, count):
    onehot = (ids[:, None] == lax.iota(jnp.int32, count)[None, :]).astype(jnp.int32)
    return jnp.sum((jnp.cumsum(onehot, axis=0) - 1) * onehot, axis=1)


def regroup(weight, gain, pieces, last):
    n_shards = lax.axis_size("fs")
    me, part = lax.axis_index("fs"), lax.axis_index("grp")
    experts, rows, cols = weight.shape
    local = experts // n_shards
    half = local // 2
    cuts = [half * i // pieces[-1] for i in pieces]
    by_dest = weight.reshape(n_shards, local, rows, cols)

    def low(block):
        if gain is not None:
            block = gain[:, None] * block
        return block.astype(jnp.bfloat16)

    own = low(lax.dynamic_index_in_dim(by_dest, me, 0, keepdims=False))
    out = jnp.broadcast_to(own[:, None], (local, n_shards, rows, cols))
    for start, end in zip(cuts[:-1], cuts[1:]):
        first = part * half + start
        theirs = (1 - part) * half + start
        send = low(lax.dynamic_slice_in_dim(by_dest, first, end - start, 1))
        if last is not None:
            send, last = lax.optimization_barrier((send, last))
        got = lax.all_to_all(send, "fs", split_axis=0, concat_axis=0, tiled=True)
        sources = [lax.rem(me + 1 + i, n_shards) for i in range(n_shards - 1)]
        remote = jnp.stack([lax.dynamic_index_in_dim(got, s, 0, keepdims=False) for s in sources])
        last = remote
        swapped = lax.ppermute(remote, "grp", [(0, 1), (1, 0)])
        out = lax.dynamic_update_slice(out, got.swapaxes(0, 1), (first, 0, 0, 0))
        for i, s in enumerate(sources):
            out = lax.dynamic_update_slice(out, swapped[i][:, None], (theirs, s, 0, 0))
    return out.reshape(local, n_shards * rows, cols), last


def grouped(tokens, norm_gain, gate_weight, up_weight, down_weight, routes, route_weights):
    experts = gate_weight.shape[0]
    n_shards = lax.axis_size("fs")
    me = lax.axis_index("fs")
    local_experts = experts // n_shards
    tok_rows = tokens.shape[0]
    room = CAP * local_experts // 2
    span = n_shards * CAP
    gate_serve, last = regroup(gate_weight, norm_gain, (0, 1), None)

    flat_routes = routes.reshape(-1)
    place = positions(flat_routes, experts).reshape(tok_rows, 2)
    row_slot = (routes % local_experts) * span + me * CAP + place
    dest = routes[:, 0] // local_experts
    seat = dest * room + positions(dest, n_shards)
    seats = lax.iota(jnp.int32, n_shards * room)
    taken = seats[:, None] == seat[None, :]
    select = taken.astype(jnp.bfloat16)
    outbound = jnp.dot(select, tokens, preferred_element_type=jnp.float32).astype(jnp.bfloat16)
    outbound = outbound.reshape(n_shards, room, outbound.shape[1])
    facts = jnp.concatenate([(row_slot + 1).astype(jnp.float32), route_weights], axis=1)
    facts = jnp.sum(jnp.where(taken[None], facts.T[:, None, :], 0.0), axis=2)
    facts = facts.reshape(4, n_shards, room).swapaxes(0, 1)
    facts, outbound, last = lax.optimization_barrier((facts, outbound, last))
    arrived = lax.all_to_all(outbound, "fs", split_axis=0, concat_axis=0, tiled=True)
    facts = lax.all_to_all(facts, "fs", split_axis=0, concat_axis=0, tiled=True)
    up_serve, last = regroup(up_weight, norm_gain, (0, 1, 2), (facts, arrived))
    down_serve, last = regroup(down_weight, None, (0, 2, 3, 4), last)
    facts = facts.swapaxes(0, 1).reshape(4, n_shards * room)
    first = facts[0].astype(jnp.int32) - 1
    second = facts[1].astype(jnp.int32) - 1
    arrived = arrived.reshape(n_shards * room, arrived.shape[2])
    normed = normalize(lax.all_gather(arrived, "tp", axis=1, tiled=True))
    slots = lax.iota(jnp.int32, local_experts * span)
    use_first = slots[None, :] == first[:, None]
    use_second = slots[None, :] == second[:, None]
    spread = (use_first | use_second).astype(jnp.bfloat16)
    expert_rows = lax.dot_general(
        spread, normed, (((0,), (0,)), ((), ())), preferred_element_type=jnp.float32
    ).astype(jnp.bfloat16)
    expert_rows = expert_rows.reshape(local_experts, span, normed.shape[1])
    gate_part = jnp.einsum(
        "erd,edh->erh", expert_rows, gate_serve, preferred_element_type=jnp.float32
    )
    up_part = jnp.einsum("erd,edh->erh", expert_rows, up_serve, preferred_element_type=jnp.float32)
    hidden = (jax.nn.silu(gate_part) * up_part).astype(jnp.bfloat16)
    expert_out = jnp.einsum(
        "erk,ekd->erd",
        lax.all_gather(hidden, "tp", axis=2, tiled=True),
        down_serve,
        preferred_element_type=jnp.float32,
    ).astype(jnp.bfloat16)
    expert_out = expert_out.reshape(local_experts * span, expert_out.shape[2])
    picked = [
        jnp.dot(use.astype(jnp.bfloat16), expert_out, preferred_element_type=jnp.float32)
        for use in (use_first, use_second)
    ]
    mixed = facts[2][:, None] * picked[0] + facts[3][:, None] * picked[1]
    mixed = mixed.astype(jnp.bfloat16).reshape(n_shards, room, expert_out.shape[1])
    back = lax.all_to_all(mixed, "fs", split_axis=0, concat_axis=0, tiled=True)
    back = back.reshape(n_shards * room, back.shape[2])
    mixture = lax.dot_general(
        select, back, (((0,), (0,)), ((), ())), preferred_element_type=jnp.float32
    ).astype(jnp.bfloat16)
    return (gate_serve, up_serve, down_serve, mixture)


def shards(tokens, norm_gain, gate_weight, up_weight, down_weight, routes, route_weights):
    experts = gate_weight.shape[0]
    n_shards = lax.axis_size("fs")
    local_experts = experts // n_shards
    if local_experts % GROUP == 0 and lax.axis_size("grp") == 2:
        return grouped(
            tokens, norm_gain, gate_weight, up_weight, down_weight, routes, route_weights
        )
    tok_rows = tokens.shape[0]
    gate_low = (norm_gain[None, :, None] * gate_weight).astype(jnp.bfloat16)
    up_low = (norm_gain[None, :, None] * up_weight).astype(jnp.bfloat16)
    down_low = down_weight.astype(jnp.bfloat16)
    gate_serve, up_serve, down_serve = (
        lax.all_to_all(gate_low, "fs", split_axis=0, concat_axis=1, tiled=True),
        lax.all_to_all(up_low, "fs", split_axis=0, concat_axis=1, tiled=True),
        lax.all_to_all(down_low, "fs", split_axis=0, concat_axis=1, tiled=True),
    )
    flat_routes = routes.reshape(-1)
    slot_index = (flat_routes * CAP + positions(flat_routes, experts)).reshape(tok_rows, 2)
    slot_ids = lax.iota(jnp.int32, experts * CAP)
    select = jnp.any(slot_ids[:, None, None] == slot_index[None, :, :], axis=2).astype(jnp.bfloat16)
    outbound = jnp.dot(select, tokens, preferred_element_type=jnp.float32).astype(jnp.bfloat16)
    outbound = outbound.reshape(n_shards, local_experts, CAP, outbound.shape[1])
    arrived = lax.all_to_all(outbound, "fs", split_axis=0, concat_axis=2, tiled=True)[0]
    expert_rows = normalize(lax.all_gather(arrived, "tp", axis=2, tiled=True))
    gate_part = jnp.einsum(
        "erd,edh->erh", expert_rows, gate_serve, preferred_element_type=jnp.float32
    )
    up_part = jnp.einsum("erd,edh->erh", expert_rows, up_serve, preferred_element_type=jnp.float32)
    hidden = (jax.nn.silu(gate_part) * up_part).astype(jnp.bfloat16)
    expert_out = jnp.einsum(
        "erk,ekd->erd",
        lax.all_gather(hidden, "tp", axis=2, tiled=True),
        down_serve,
        preferred_element_type=jnp.float32,
    ).astype(jnp.bfloat16)
    expert_out = expert_out.reshape(1, local_experts, hidden.shape[1], expert_out.shape[2])
    returned_rows = lax.all_to_all(expert_out, "fs", split_axis=2, concat_axis=0, tiled=True)
    returned_rows = returned_rows.reshape(experts * CAP, returned_rows.shape[3])
    picked = returned_rows[slot_index]
    mixture = jnp.sum(route_weights[:, :, None] * picked.astype(jnp.float32), axis=1).astype(
        jnp.bfloat16
    )
    return (gate_serve, up_serve, down_serve, mixture)


def solution(mesh):
    in_specs = (
        P(("grp", "fs"), "tp"),
        P("fs"),
        P(None, "fs", "tp"),
        P(None, "fs", "tp"),
        P(None, "fs", "tp"),
        P(("grp", "fs"), None),
        P(("grp", "fs"), None),
    )
    out_specs = (
        P(("grp", "fs"), None, "tp"),
        P(("grp", "fs"), None, "tp"),
        P(("grp", "fs"), None, "tp"),
        P(("grp", "fs"), "tp"),
    )
    return jax.shard_map(shards, mesh=mesh, in_specs=in_specs, out_specs=out_specs, check_vma=False)
```

```python
import jax
import jax.numpy as jnp
from jax import lax
from jax.sharding import PartitionSpec as P

CAP = 36
GROUP = 8


epsilon = 1e-06


def normalize(rows):
    values = rows.astype(jnp.float32)
    scale = lax.rsqrt(jnp.mean(values * values, axis=-1, keepdims=True) + epsilon)
    return (values * scale).astype(jnp.bfloat16)


def positions(ids, count):
    onehot = (ids[:, None] == lax.iota(jnp.int32, count)[None, :]).astype(jnp.int32)
    return jnp.sum((jnp.cumsum(onehot, axis=0) - 1) * onehot, axis=1)


def shift(block, axis, step):
    size = lax.axis_size(axis)
    return lax.ppermute(block, axis, [(i, (i + step) % size) for i in range(size)])


def spread_blocks(blocks, axis, sign):
    return [blocks[0]] + [shift(blocks[i], axis, i * sign) for i in range(1, len(blocks))]


def gather_last(block, axis):
    size, me = lax.axis_size(axis), lax.axis_index(axis)
    width = block.shape[-1]
    whole = jnp.zeros(block.shape[:-1] + (size * width,), block.dtype)
    for i, held in enumerate(spread_blocks([block] * size, axis, 1)):
        start = lax.rem(me - i + size, size) * width
        whole = lax.dynamic_update_slice_in_dim(whole, held, start, whole.ndim - 1)
    return whole


def regroup(weight, gain, pieces, last, moves):
    n_shards = lax.axis_size("fs")
    me, part = lax.axis_index("fs"), lax.axis_index("grp")
    experts, rows, cols = weight.shape
    local = experts // n_shards
    half = local // 2
    cuts = [half * i // pieces[-1] for i in pieces]
    by_dest = weight.reshape(n_shards, local, rows, cols)

    def low(block):
        if gain is not None:
            block = gain[:, None] * block
        return block.astype(jnp.bfloat16)

    own = low(lax.dynamic_index_in_dim(by_dest, me, 0, keepdims=False))
    out = jnp.broadcast_to(own[:, None], (local, n_shards, rows, cols))
    for start, end in zip(cuts[:-1], cuts[1:]):
        first = part * half + start
        theirs = (1 - part) * half + start
        send = low(lax.dynamic_slice_in_dim(by_dest, first, end - start, 1))
        if last is not None:
            send, last = lax.optimization_barrier((send, last))
        got = lax.all_to_all(send, "fs", split_axis=0, concat_axis=0, tiled=True)
        sources = [lax.rem(me + 1 + i, n_shards) for i in range(n_shards - 1)]
        remote = jnp.stack([lax.dynamic_index_in_dim(got, s, 0, keepdims=False) for s in sources])
        last = remote
        swapped = lax.ppermute(remote, "grp", [(0, 1), (1, 0)])
        moves.append(first)
        out = lax.dynamic_update_slice(out, got.swapaxes(0, 1), (first, 0, 0, 0))
        for i, s in enumerate(sources):
            out = lax.dynamic_update_slice(out, swapped[i][:, None], (theirs, s, 0, 0))
    return out.reshape(local, n_shards * rows, cols), last


def grouped(tokens, norm_gain, gate_weight, up_weight, down_weight, routes, route_weights):
    experts = gate_weight.shape[0]
    n_shards = lax.axis_size("fs")
    me = lax.axis_index("fs")
    local_experts = experts // n_shards
    tok_rows = tokens.shape[0]
    room = CAP * local_experts // 2
    span = n_shards * CAP
    moves = []
    gate_serve, last = regroup(gate_weight, norm_gain, (0, 1, 2), None, moves)
    up_serve, last = regroup(up_weight, norm_gain, (0, 1, 2), last, moves)
    down_serve, last = regroup(down_weight, None, (0, 2, 3, 4), last, moves)

    flat_routes = routes.reshape(-1)
    place = positions(flat_routes, experts).reshape(tok_rows, 2)
    row_slot = (routes % local_experts) * span + me * CAP + place
    dest = routes[:, 0] // local_experts
    ahead = lax.rem(dest - me + n_shards, n_shards)
    seat = ahead * room + positions(dest, n_shards)
    seats = lax.iota(jnp.int32, n_shards * room)
    taken = seats[:, None] == seat[None, :]
    select = taken.astype(jnp.bfloat16)
    outbound = jnp.dot(select, tokens, preferred_element_type=jnp.float32).astype(jnp.bfloat16)
    outbound = outbound.reshape(n_shards, room, outbound.shape[1])
    facts = jnp.concatenate([(row_slot + 1).astype(jnp.float32), route_weights], axis=1)
    facts = jnp.sum(jnp.where(taken[None], facts.T[:, None, :], 0.0), axis=2)
    facts = facts.reshape(4, n_shards, room).swapaxes(0, 1)
    facts = jnp.concatenate(spread_blocks(list(facts), "fs", 1), axis=1)
    arrived = jnp.concatenate(spread_blocks(list(outbound), "fs", 1), axis=0)
    first = facts[0].astype(jnp.int32) - 1
    second = facts[1].astype(jnp.int32) - 1
    whole_rows = gather_last(arrived, "tp")
    normed = normalize(whole_rows)
    slots = lax.iota(jnp.int32, local_experts * span)
    use_first = slots[None, :] == first[:, None]
    use_second = slots[None, :] == second[:, None]
    spread = (use_first | use_second).astype(jnp.bfloat16)
    expert_rows = lax.dot_general(
        spread, normed, (((0,), (0,)), ((), ())), preferred_element_type=jnp.float32
    ).astype(jnp.bfloat16)
    expert_rows = expert_rows.reshape(local_experts, span, normed.shape[1])
    gate_part = jnp.einsum(
        "erd,edh->erh", expert_rows, gate_serve, preferred_element_type=jnp.float32
    )
    up_part = jnp.einsum("erd,edh->erh", expert_rows, up_serve, preferred_element_type=jnp.float32)
    hidden = (jax.nn.silu(gate_part) * up_part).astype(jnp.bfloat16)
    expert_out = jnp.einsum(
        "erk,ekd->erd",
        gather_last(hidden, "tp"),
        down_serve,
        preferred_element_type=jnp.float32,
    ).astype(jnp.bfloat16)
    expert_out = expert_out.reshape(local_experts * span, expert_out.shape[2])
    picked = [
        jnp.dot(use.astype(jnp.bfloat16), expert_out, preferred_element_type=jnp.float32)
        for use in (use_first, use_second)
    ]
    mixed = facts[2][:, None] * picked[0] + facts[3][:, None] * picked[1]
    mixed = mixed.astype(jnp.bfloat16).reshape(n_shards, room, expert_out.shape[1])
    back = jnp.concatenate(spread_blocks(list(mixed), "fs", -1), axis=0)
    mixture = lax.dot_general(
        select, back, (((0,), (0,)), ((), ())), preferred_element_type=jnp.float32
    ).astype(jnp.bfloat16)
    return (gate_serve, up_serve, down_serve, mixture)


def shards(tokens, norm_gain, gate_weight, up_weight, down_weight, routes, route_weights):
    experts = gate_weight.shape[0]
    n_shards = lax.axis_size("fs")
    local_experts = experts // n_shards
    if local_experts % GROUP == 0 and lax.axis_size("grp") == 2:
        return grouped(
            tokens, norm_gain, gate_weight, up_weight, down_weight, routes, route_weights
        )
    tok_rows = tokens.shape[0]
    gate_low = (norm_gain[None, :, None] * gate_weight).astype(jnp.bfloat16)
    up_low = (norm_gain[None, :, None] * up_weight).astype(jnp.bfloat16)
    down_low = down_weight.astype(jnp.bfloat16)
    gate_serve, up_serve, down_serve = (
        lax.all_to_all(gate_low, "fs", split_axis=0, concat_axis=1, tiled=True),
        lax.all_to_all(up_low, "fs", split_axis=0, concat_axis=1, tiled=True),
        lax.all_to_all(down_low, "fs", split_axis=0, concat_axis=1, tiled=True),
    )
    flat_routes = routes.reshape(-1)
    slot_index = (flat_routes * CAP + positions(flat_routes, experts)).reshape(tok_rows, 2)
    slot_ids = lax.iota(jnp.int32, experts * CAP)
    select = jnp.any(slot_ids[:, None, None] == slot_index[None, :, :], axis=2).astype(jnp.bfloat16)
    outbound = jnp.dot(select, tokens, preferred_element_type=jnp.float32).astype(jnp.bfloat16)
    outbound = outbound.reshape(n_shards, local_experts, CAP, outbound.shape[1])
    arrived = lax.all_to_all(outbound, "fs", split_axis=0, concat_axis=2, tiled=True)[0]
    expert_rows = normalize(lax.all_gather(arrived, "tp", axis=2, tiled=True))
    gate_part = jnp.einsum(
        "erd,edh->erh", expert_rows, gate_serve, preferred_element_type=jnp.float32
    )
    up_part = jnp.einsum("erd,edh->erh", expert_rows, up_serve, preferred_element_type=jnp.float32)
    hidden = (jax.nn.silu(gate_part) * up_part).astype(jnp.bfloat16)
    expert_out = jnp.einsum(
        "erk,ekd->erd",
        lax.all_gather(hidden, "tp", axis=2, tiled=True),
        down_serve,
        preferred_element_type=jnp.float32,
    ).astype(jnp.bfloat16)
    expert_out = expert_out.reshape(1, local_experts, hidden.shape[1], expert_out.shape[2])
    returned_rows = lax.all_to_all(expert_out, "fs", split_axis=2, concat_axis=0, tiled=True)
    returned_rows = returned_rows.reshape(experts * CAP, returned_rows.shape[3])
    picked = returned_rows[slot_index]
    mixture = jnp.sum(route_weights[:, :, None] * picked.astype(jnp.float32), axis=1).astype(
        jnp.bfloat16
    )
    return (gate_serve, up_serve, down_serve, mixture)


def solution(mesh):
    in_specs = (
        P(("grp", "fs"), "tp"),
        P("fs"),
        P(None, "fs", "tp"),
        P(None, "fs", "tp"),
        P(None, "fs", "tp"),
        P(("grp", "fs"), None),
        P(("grp", "fs"), None),
    )
    out_specs = (
        P(("grp", "fs"), None, "tp"),
        P(("grp", "fs"), None, "tp"),
        P(("grp", "fs"), None, "tp"),
        P(("grp", "fs"), "tp"),
    )
    return jax.shard_map(shards, mesh=mesh, in_specs=in_specs, out_specs=out_specs, check_vma=False)
```
